32 devices in a mesh: grp: 2 (over y), fs: 4 (over z), tp: 4 (over x, core).
Axes of the slice: x: 2, y: 2, z: 4, core: 2. Of those that a mesh axis runs over, the one named last changes fastest.
Arguments:
- stream: bfloat16 [2048, 3072], P('tp', ('grp', 'fs')), parts along dimension 1, may hold values from -6 to 6
- first_gain: float32 [2048], replicated, may hold values from 0.1 to 1.9
- first_gate: float32 [2048, 5632], P('fs', 'tp'), may hold values from -0.125 to 0.125
- first_gate_scale: float32 [5632], P('tp'), may hold values from 0.5 to 2
- first_up: float32 [2048, 5632], P('fs', 'tp'), may hold values from -0.125 to 0.125
- first_up_scale: float32 [5632], P('tp'), may hold values from 0.5 to 2
- first_down: float32 [5632, 2048], P('tp', 'fs'), may hold values from -0.078125 to 0.078125
- first_down_scale: float32 [2048], P('fs'), may hold values from 0.5 to 2
- mixer_gain: float32 [2048], replicated, may hold values from 0.1 to 1.9
- mixer_left: float32 [2048, 1024], P('fs', 'tp'), may hold values from -0.125 to 0.125
- mixer_left_scale: float32 [1024], P('tp'), may hold values from 0.5 to 2
- mixer_right: float32 [2048, 1024], P('fs', 'tp'), may hold values from -0.125 to 0.125
- mixer_right_scale: float32 [1024], P('tp'), may hold values from 0.5 to 2
- channel_gain: float32 [1024], P('tp'), may hold values from 0.1 to 1.9
- spatial: bfloat16 [8, 128, 128], P('tp'), may hold values from -0.5 to 0.5
- spatial_bias: float32 [8, 128], P('tp'), may hold values from 0.1 to 1.9
- mixer_out: float32 [1024, 2048], P('tp', 'fs'), may hold values from -0.1875 to 0.1875
- mixer_out_scale: float32 [2048], P('fs'), may hold values from 0.5 to 2
- second_gain: float32 [2048], replicated, may hold values from 0.1 to 1.9
- second_gate: float32 [2048, 5632], P('fs', 'tp'), may hold values from -0.125 to 0.125
- second_gate_scale: float32 [5632], P('tp'), may hold values from 0.5 to 2
- second_up: float32 [2048, 5632], P('fs', 'tp'), may hold values from -0.125 to 0.125
- second_up_scale: float32 [5632], P('tp'), may hold values from 0.5 to 2
- second_down: float32 [5632, 2048], P('tp', 'fs'), may hold values from -0.078125 to 0.078125
- second_down_scale: float32 [2048], P('fs'), may hold values from 0.5 to 2
Outputs:
- result: bfloat16 [2048, 3072], P('tp', ('grp', 'fs')), parts along dimension 1
The draws below stay inside these ranges and needn't reach their ends.
There are 2 independent parts, one for each index of `grp`. The reference program is written for one: setup_inputs(seed, part) draws one part's arguments, and reference() takes and returns one part's arrays. A program takes and returns all parts, laid end to end along the dimension named above; an argument that names none is the same for every part. Nothing has to cross between parts.
All inputs are finite; a program needn't handle non-finite values.
Results may differ from the reference program's by a relative error of at most 0.02.
Values may be sent and summed in bfloat16 or wider, within the bound.
A program may use at most 128 MiB of HBM per device.

```python
import math
import jax
import jax.numpy as jnp
from jax import lax

D = 2048
FF = 5632
BRANCH = 1024
GROUPS = 8
BLOCK = 128
TOKENS = 1536
N_TP = 4


def steps_of(rng, dims, split, least, largest):
    def one(axis_at, shards_of):
        draws = jax.random.uniform(jax.random.fold_in(jax.random.fold_in(rng, 6), axis_at), (shards_of,), jnp.float32, least / len(split), largest / len(split))
        return jnp.repeat(jnp.exp(draws), dims[axis_at] // shards_of).reshape((-1,) + (1,) * (len(dims) - axis_at - 1))

    level = one(*split[0])
    for cut in split[1:]:
        level = level * one(*cut)
    return level


def normal_values(own_key, shape, scale, most, split=(), kind=jnp.bfloat16):
    values = jax.random.normal(own_key, shape, jnp.float32) * scale
    if len(split) > 0:
        values = steps_of(own_key, shape, split, -0.22, 0.18) * values
    return jnp.clip(values, min=-most, max=most).astype(kind)


def setup_inputs(seed: int = 0, part: int = 0) -> dict:
    key_of = jax.random.split(jax.random.key(seed), 26)
    own_keys = jax.random.split(jax.random.fold_in(key_of[25], part), 26)
    return {
        "stream": normal_values(own_keys[0], (D, TOKENS), 1.0, 6.0, ((0, 4), (1, 4))),
        "first_gain": jnp.clip(1.0 + 0.18 * jax.random.normal(key_of[1], (D,), jnp.float32), 0.1, 1.9),
        "first_gate": normal_values(key_of[2], (D, FF), D ** -0.5, 0.125, ((0, 4), (1, 4)), jnp.float32),
        "first_gate_scale": jnp.clip(jnp.exp(math.log(2.0) - 1.3862944 * jax.random.uniform(key_of[3], (FF,), jnp.float32) ** steps_of(key_of[3], (FF,), ((0, 4),), -0.2, 0.2)), 0.5, 2.0),
        "first_up": normal_values(key_of[4], (D, FF), D ** -0.5, 0.125, ((0, 4), (1, 4)), jnp.float32),
        "first_up_scale": jnp.clip(jnp.exp(math.log(2.0) - 1.3862944 * jax.random.uniform(key_of[5], (FF,), jnp.float32) ** steps_of(key_of[5], (FF,), ((0, 4),), -0.2, 0.2)), 0.5, 2.0),
        "first_down": normal_values(key_of[6], (FF, D), FF ** -0.5, 0.078125, ((0, 4), (1, 4)), jnp.float32),
        "first_down_scale": jnp.clip(jnp.exp(math.log(2.0) - 1.3862944 * jax.random.uniform(key_of[7], (D,), jnp.float32) ** steps_of(key_of[7], (D,), ((0, 4),), -0.2, 0.2)), 0.5, 2.0),
        "mixer_gain": jnp.clip(1.0 + 0.18 * jax.random.normal(key_of[8], (D,), jnp.float32), 0.1, 1.9),
        "mixer_left": normal_values(key_of[9], (D, BRANCH), D ** -0.5, 0.125, ((0, 4), (1, 4)), jnp.float32),
        "mixer_left_scale": jnp.clip(jnp.exp(math.log(2.0) - 1.3862944 * jax.random.uniform(key_of[10], (BRANCH,), jnp.float32) ** steps_of(key_of[10], (BRANCH,), ((0, 4),), -0.2, 0.2)), 0.5, 2.0),
        "mixer_right": normal_values(key_of[11], (D, BRANCH), D ** -0.5, 0.125, ((0, 4), (1, 4)), jnp.float32),
        "mixer_right_scale": jnp.clip(jnp.exp(math.log(2.0) - 1.3862944 * jax.random.uniform(key_of[12], (BRANCH,), jnp.float32) ** steps_of(key_of[12], (BRANCH,), ((0, 4),), -0.2, 0.2)), 0.5, 2.0),
        "channel_gain": jnp.clip(1.0 + 0.18 * jax.random.normal(key_of[13], (BRANCH,), jnp.float32), 0.1, 1.9),
        "spatial": normal_values(key_of[14], (GROUPS, BLOCK, BLOCK), BLOCK ** -0.5, 0.5, ((0, 4),)),
        "spatial_bias": jnp.clip(1.0 + 0.18 * jax.random.normal(key_of[15], (GROUPS, BLOCK), jnp.float32), 0.1, 1.9),
        "mixer_out": normal_values(key_of[16], (BRANCH, D), BRANCH ** -0.5, 0.1875, ((0, 4), (1, 4)), jnp.float32),
        "mixer_out_scale": jnp.clip(jnp.exp(math.log(2.0) - 1.3862944 * jax.random.uniform(key_of[17], (D,), jnp.float32) ** steps_of(key_of[17], (D,), ((0, 4),), -0.2, 0.2)), 0.5, 2.0),
        "second_gain": jnp.clip(1.0 + 0.18 * jax.random.normal(key_of[18], (D,), jnp.float32), 0.1, 1.9),
        "second_gate": normal_values(key_of[19], (D, FF), D ** -0.5, 0.125, ((0, 4), (1, 4)), jnp.float32),
        "second_gate_scale": jnp.clip(jnp.exp(math.log(2.0) - 1.3862944 * jax.random.uniform(key_of[20], (FF,), jnp.float32) ** steps_of(key_of[20], (FF,), ((0, 4),), -0.2, 0.2)), 0.5, 2.0),
        "second_up": normal_values(key_of[21], (D, FF), D ** -0.5, 0.125, ((0, 4), (1, 4)), jnp.float32),
        "second_up_scale": jnp.clip(jnp.exp(math.log(2.0) - 1.3862944 * jax.random.uniform(key_of[22], (FF,), jnp.float32) ** steps_of(key_of[22], (FF,), ((0, 4),), -0.2, 0.2)), 0.5, 2.0),
        "second_down": normal_values(key_of[23], (FF, D), FF ** -0.5, 0.078125, ((0, 4), (1, 4)), jnp.float32),
        "second_down_scale": jnp.clip(jnp.exp(math.log(2.0) - 1.3862944 * jax.random.uniform(key_of[24], (D,), jnp.float32) ** steps_of(key_of[24], (D,), ((0, 4),), -0.2, 0.2)), 0.5, 2.0),
    }


EPS = 1e-06

def rms_rows(stream, gain):
    values = stream.astype(jnp.float32)
    inverse = lax.rsqrt(lax.optimization_barrier(jnp.mean(values * values, axis=0)) + EPS)
    return (values * inverse * gain[:, None]).astype(jnp.bfloat16)

def project(weight, scale, inputs):
    product = lax.dot_general(weight.astype(jnp.bfloat16), inputs, (((0,), (0,)), ((), ())), preferred_element_type=jnp.float32)
    return product * scale[:, None]

def block_sum(weight, scale, hidden):
    width = weight.shape[0] // N_TP
    total = jnp.zeros((weight.shape[1], hidden.shape[1]), jnp.float32)
    for index in range(N_TP):
        term = project(weight[index * width:(index + 1) * width], scale, hidden[index * width:(index + 1) * width])
        total = total + lax.optimization_barrier(term.astype(jnp.bfloat16)).astype(jnp.float32)
    return total

def half_step(stream, gain, gate_weight, gate_scale, up_weight, up_scale, down_weight, down_scale):
    normed_rows = rms_rows(stream, gain)
    gate = project(gate_weight, gate_scale, normed_rows)
    upward = project(up_weight, up_scale, normed_rows)
    hidden = (jax.nn.silu(gate) * upward).astype(jnp.bfloat16)
    total = block_sum(down_weight, down_scale, hidden)
    return (stream.astype(jnp.float32) + 0.5 * total).astype(jnp.bfloat16)

def reference(stream, first_gain, first_gate, first_gate_scale, first_up, first_up_scale, first_down, first_down_scale, mixer_gain, mixer_left, mixer_left_scale, mixer_right, mixer_right_scale, channel_gain, spatial, spatial_bias, mixer_out, mixer_out_scale, second_gain, second_gate, second_gate_scale, second_up, second_up_scale, second_down, second_down_scale):
    stream = half_step(stream, first_gain, first_gate, first_gate_scale, first_up, first_up_scale, first_down, first_down_scale)
    normed_rows = rms_rows(stream, mixer_gain)
    left = jax.nn.gelu(project(mixer_left, mixer_left_scale, normed_rows))
    right = jax.nn.gelu(project(mixer_right, mixer_right_scale, normed_rows))
    average = lax.optimization_barrier(jnp.mean(right, axis=0))
    squares = lax.optimization_barrier(jnp.mean(right * right, axis=0))
    inverse = lax.rsqrt(squares - average * average + EPS)
    centred = ((right - average) * inverse * channel_gain[:, None]).astype(jnp.bfloat16)
    blocks = centred.reshape(GROUPS, BRANCH // GROUPS, TOKENS // BLOCK, BLOCK)
    lower = jnp.tril(jnp.ones((BLOCK, BLOCK), dtype=bool))
    masked = jnp.where(lower[None], spatial, jnp.zeros_like(spatial))
    token_mix = jnp.einsum('gts,gcns->gcnt', masked.astype(jnp.float32), blocks.astype(jnp.float32))
    token_mix = token_mix + spatial_bias[:, None, None, :]
    gated = (left * token_mix.reshape(BRANCH, TOKENS)).astype(jnp.bfloat16)
    total = block_sum(mixer_out, mixer_out_scale, gated)
    stream = (stream.astype(jnp.float32) + total).astype(jnp.bfloat16)
    return half_step(stream, second_gain, second_gate, second_gate_scale, second_up, second_up_scale, second_down, second_down_scale)
```

```python
import jax
import jax.numpy as jnp
from jax import lax
from jax.sharding import PartitionSpec as P


BRANCH = 1024


EPS = 1e-06
LAST_PARTS = 2


def contract(left_side, right_side):
    return lax.dot_general(
        left_side, right_side, (((0,), (0,)), ((), ())), preferred_element_type=jnp.float32
    )


CORES = 2


def shifted(block, axis_name, step):
    count = lax.axis_size(axis_name)
    return lax.ppermute(block, axis_name, [(at, (at + step) % count) for at in range(count)])


def to_same_core(block, step):
    count = lax.axis_size("tp")
    return lax.ppermute(
        block, "tp", [(at, (at + step * CORES) % count) for at in range(count)]
    )


def to_other_core(block):
    return lax.ppermute(block, "tp", [(at, at ^ 1) for at in range(lax.axis_size("tp"))])


def pick(blocks, index):
    count = len(blocks)
    if count == 1:
        return blocks[0]
    index = lax.rem(index + count, count)
    found = blocks[0]
    for at in range(1, count):
        found = jnp.where(index == at, blocks[at], found)
    return found


def chip_and_core():
    place = lax.axis_index("tp")
    return lax.div(place, CORES), lax.rem(place, CORES)


def gather_rows(block):
    chips = lax.axis_size("tp") // CORES
    chip, core = chip_and_core()
    held = jnp.stack([block] + [to_same_core(block, step) for step in range(1, chips)])
    other = to_other_core(held)
    found = []
    for at_chip in range(chips):
        mine = pick([held[step] for step in range(chips)], chip - at_chip)
        theirs = pick([other[step] for step in range(chips)], chip - at_chip)
        found += [jnp.where(core == 0, mine, theirs), jnp.where(core == 0, theirs, mine)]
    return jnp.concatenate(found)


def scatter_sum(terms):
    chips = lax.axis_size("tp") // CORES
    chip, core = chip_and_core()
    blocks = terms.reshape((chips, CORES, -1) + terms.shape[1:])
    mine = jnp.where(core == 0, blocks[:, 0], blocks[:, 1])
    passed = jnp.where(core == 0, blocks[:, 1], blocks[:, 0])
    pairs = mine.astype(jnp.float32) + to_other_core(passed).astype(jnp.float32)
    total = pick([pairs[at] for at in range(chips)], chip)
    for step in range(1, chips):
        sent = pick([pairs[at] for at in range(chips)], chip + step).astype(jnp.bfloat16)
        total = total + to_same_core(sent, step).astype(jnp.float32)
    return total


def share_of(weight_part, axis, back):
    shares = lax.axis_size("grp")
    width = weight_part.shape[axis] // shares
    index = lax.rem(lax.axis_index("grp") - back + shares, shares)
    return lax.dynamic_slice_in_dim(weight_part, index * width, width, axis).astype(jnp.bfloat16)


def ring_place(step):
    return lax.rem(lax.axis_index("fs") + step, lax.axis_size("fs"))


def exchange(share, following):
    blocks = lax.all_gather(share, "fs", axis=0, tiled=False)
    rest = jnp.stack(
        [
            lax.dynamic_index_in_dim(blocks, ring_place(step), 0, keepdims=False)
            for step in range(1, lax.axis_size("fs"))
        ]
    )
    if following is not None:
        rest, following = lax.optimization_barrier((rest, following))
    rests = [shifted(rest, "grp", back) for back in range(1, lax.axis_size("grp"))]
    return blocks, rests, following


def flat(blocks):
    return blocks.reshape((-1,) + blocks.shape[2:])


def joined(blocks, rests, locals_of):
    pieces = [flat(blocks)]
    for rest, own in zip(rests, locals_of):
        pieces += [own, flat(rest)]
    return jnp.concatenate(pieces)


def rows_in_order(normed_rows):
    shares, count = (lax.axis_size("grp"), lax.axis_size("fs"))
    rows = normed_rows.reshape(count, shares, -1, normed_rows.shape[1])

    def at(place, back):
        index = lax.rem(lax.axis_index("grp") - back + shares, shares)
        return lax.dynamic_slice(
            rows, (place, index, 0, 0), (1, 1, rows.shape[2], rows.shape[3])
        ).reshape(rows.shape[2:])

    pieces = [at(place, 0) for place in range(count)]
    for back in range(1, shares):
        pieces += [at(ring_place(step), back) for step in range(count)]
    return jnp.concatenate(pieces)


def column_terms(blocks, rests, locals_of, scale, hidden, transposed):
    shares, count = (lax.axis_size("grp"), lax.axis_size("fs"))
    place = lax.axis_index("fs")

    def product(pieces):
        form = "bnk,kt->bnt" if transposed else "bkn,kt->bnt"
        return jnp.einsum(form, pieces, hidden, preferred_element_type=jnp.float32)

    def scale_at(back):
        index = lax.rem(lax.axis_index("grp") - back + shares, shares)
        return lax.dynamic_index_in_dim(scale, index, 1, keepdims=False)[:, :, None]

    own = (product(blocks) * scale_at(0)).astype(jnp.bfloat16)
    found = [[own[at] for at in range(count)]]
    for back in range(1, shares):
        turned = scale_at(back)
        here = lax.dynamic_index_in_dim(turned, place, 0)
        local = (product(locals_of[back - 1][None]) * here).astype(jnp.bfloat16)
        away = jnp.stack(
            [
                lax.dynamic_index_in_dim(turned, ring_place(step), 0, keepdims=False)
                for step in range(1, count)
            ]
        )
        rest = (product(rests[back - 1]) * away).astype(jnp.bfloat16)
        ring = [local[0]] + [rest[at] for at in range(count - 1)]
        found.append([pick(ring, at - place) for at in range(count)])
    grp = lax.axis_index("grp")
    return [
        [pick([found[back][at] for back in range(shares)], grp - share) for share in range(shares)]
        for at in range(count)
    ]


def normed(stream, gain):
    whole_rows = gather_rows(stream)
    values = whole_rows.astype(jnp.float32)
    inverse = lax.rsqrt(jnp.mean(values * values, axis=0) + EPS)
    return (values * inverse * gain[:, None]).astype(jnp.bfloat16)


def residual(stream, total, factor):
    return (stream.astype(jnp.float32) + factor * total).astype(jnp.bfloat16)


def swish_hidden(gate, gate_scale, upward, up_scale):
    return (jax.nn.silu(gate * gate_scale[:, None]) * (upward * up_scale[:, None])).astype(
        jnp.bfloat16
    )


def gating_unit(left_pre, right_pre, channel_gain, spatial, spatial_bias):
    left = jax.nn.gelu(left_pre)
    right = jax.nn.gelu(right_pre)
    totals, squares = lax.psum((jnp.sum(right, axis=0), jnp.sum(right * right, axis=0)), "tp")
    average = totals / BRANCH
    inverse = lax.rsqrt(squares / BRANCH - average * average + EPS)
    centred = ((right - average) * inverse * channel_gain[:, None]).astype(jnp.bfloat16)
    local_groups, span = (spatial.shape[0], spatial.shape[1])
    tokens = centred.shape[1]
    blocks = centred.reshape(local_groups, centred.shape[0] // local_groups, tokens // span, span)
    target = lax.broadcasted_iota(jnp.int32, (span, span), 0)
    source = lax.broadcasted_iota(jnp.int32, (span, span), 1)
    masked = jnp.where((source <= target)[None], spatial, jnp.zeros_like(spatial))
    token_mix = jnp.einsum("gts,gcns->gcnt", masked, blocks, preferred_element_type=jnp.float32)
    token_mix = token_mix + spatial_bias[:, None, None, :]
    return (left * token_mix.reshape(centred.shape[0], tokens)).astype(jnp.bfloat16)


def layer(
    stream,
    first_gain,
    first_gate,
    first_gate_scale,
    first_up,
    first_up_scale,
    first_down,
    first_down_scale,
    mixer_gain,
    mixer_left,
    mixer_left_scale,
    mixer_right,
    mixer_right_scale,
    channel_gain,
    spatial,
    spatial_bias,
    mixer_out,
    mixer_out_scale,
    second_gain,
    second_gate,
    second_gate_scale,
    second_up,
    second_up_scale,
    second_down,
    second_down_scale,
):
    shares, count = (lax.axis_size("grp"), lax.axis_size("fs"))
    backs = range(1, shares)
    cols = lax.all_gather(
        jnp.stack([first_down_scale, mixer_out_scale, second_down_scale]), "fs", axis=0, tiled=False
    )
    cols = cols.reshape(count, 3, shares, -1)

    def mixer_share(back):
        return jnp.stack(
            [
                share_of(mixer_left, 0, back),
                share_of(mixer_right, 0, back),
                share_of(mixer_out, 1, back).T,
            ]
        )

    def rows_share(weight):
        return lambda back: share_of(weight, 0, back)

    def cols_share(weight, part, parts):
        def cut(back):
            share = share_of(weight, 1, back)
            width = share.shape[1] // parts
            return share[:, part * width : (part + 1) * width]

        return cut

    units = (
        rows_share(first_gate),
        rows_share(first_up),
        cols_share(first_down, 0, 1),
        mixer_share,
        rows_share(second_gate),
        rows_share(second_up),
    ) + tuple(cols_share(second_down, part, LAST_PARTS) for part in range(LAST_PARTS))
    ready = []
    share = units[0](0)
    for number, unit in enumerate(units):
        following = units[number + 1](0) if number + 1 < len(units) else None
        blocks, rests, share = exchange(share, following)
        ready.append((blocks, rests, [unit(back) for back in backs]))

    def half_step(stream, gain, gate_unit, gate_scale, up_unit, up_scale, down_units, down_cols):
        rows = rows_in_order(normed(stream, gain))
        gate = contract(joined(*gate_unit), rows)
        upward = contract(joined(*up_unit), rows)
        hidden = swish_hidden(gate, gate_scale, upward, up_scale)
        width = down_cols.shape[2] // len(down_units)
        terms = [
            column_terms(
                *unit, down_cols[:, :, part * width : (part + 1) * width], hidden, False
            )
            for part, unit in enumerate(down_units)
        ]
        ordered = [
            term[at][share] for at in range(count) for share in range(shares) for term in terms
        ]
        return residual(stream, scatter_sum(jnp.concatenate(ordered)), 0.5)

    stream = half_step(
        stream, first_gain, ready[0], first_gate_scale, ready[1], first_up_scale, ready[2:3], cols[:, 0]
    )
    rows = rows_in_order(normed(stream, mixer_gain))
    blocks, rests, local_shares = ready[3]

    def mixer_unit(index):
        return (
            blocks[:, index],
            [rest[:, index] for rest in rests],
            [local_share[index] for local_share in local_shares],
        )

    left_pre = contract(joined(*mixer_unit(0)), rows)
    right_pre = contract(joined(*mixer_unit(1)), rows)
    gated = gating_unit(
        left_pre * mixer_left_scale[:, None],
        right_pre * mixer_right_scale[:, None],
        channel_gain,
        spatial,
        spatial_bias,
    )
    terms = column_terms(*mixer_unit(2), cols[:, 1], gated, True)
    terms = jnp.concatenate([terms[at][share] for at in range(count) for share in range(shares)])
    stream = residual(stream, scatter_sum(terms), 1.0)
    return half_step(
        stream, second_gain, ready[4], second_gate_scale, ready[5], second_up_scale, ready[6:], cols[:, 2]
    )


def solution(mesh):
    return jax.shard_map(
        layer,
        mesh=mesh,
        in_specs=(
            P("tp", ("grp", "fs")),
            P(),
            P("fs", "tp"),
            P("tp"),
            P("fs", "tp"),
            P("tp"),
            P("tp", "fs"),
            P("fs"),
            P(),
            P("fs", "tp"),
            P("tp"),
            P("fs", "tp"),
            P("tp"),
            P("tp"),
            P("tp", None, None),
            P("tp", None),
            P("tp", "fs"),
            P("fs"),
            P(),
            P("fs", "tp"),
            P("tp"),
            P("fs", "tp"),
            P("tp"),
            P("tp", "fs"),
            P("fs"),
        ),
        out_specs=P("tp", ("grp", "fs")),
        check_vma=False,
    )
```

```python
import jax
import jax.numpy as jnp
from jax import lax
from jax.sharding import PartitionSpec as P


BRANCH = 1024


EPS = 1e-06
LAST_PARTS = 2


def contract(left_side, right_side):
    return lax.dot_general(
        left_side, right_side, (((0,), (0,)), ((), ())), preferred_element_type=jnp.float32
    )


CORES = 2


def shifted(block, axis_name, step):
    count = lax.axis_size(axis_name)
    return lax.ppermute(block, axis_name, [(at, (at + step) % count) for at in range(count)])


def to_same_core(block, step):
    count = lax.axis_size("tp")
    return lax.ppermute(
        block, "tp", [(at, (at + step * CORES) % count) for at in range(count)]
    )


def to_other_core(block):
    return lax.ppermute(block, "tp", [(at, at ^ 1) for at in range(lax.axis_size("tp"))])


def pick(blocks, index):
    count = len(blocks)
    if count == 1:
        return blocks[0]
    index = lax.rem(index + count, count)
    found = blocks[0]
    for at in range(1, count):
        found = jnp.where(index == at, blocks[at], found)
    return found


def chip_and_core():
    place = lax.axis_index("tp")
    return lax.div(place, CORES), lax.rem(place, CORES)


def gather_rows(block):
    chips = lax.axis_size("tp") // CORES
    chip, core = chip_and_core()
    held = jnp.stack([block] + [to_same_core(block, step) for step in range(1, chips)])
    other = to_other_core(held)
    found = []
    for at_chip in range(chips):
        mine = pick([held[step] for step in range(chips)], chip - at_chip)
        theirs = pick([other[step] for step in range(chips)], chip - at_chip)
        found += [jnp.where(core == 0, mine, theirs), jnp.where(core == 0, theirs, mine)]
    return jnp.concatenate(found)


def scatter_blocks(terms):
    chips = lax.axis_size("tp") // CORES
    chip, core = chip_and_core()
    blocks = terms.reshape((chips, CORES, -1) + terms.shape[1:])
    mine = jnp.where(core == 0, blocks[:, 0], blocks[:, 1])
    passed = jnp.where(core == 0, blocks[:, 1], blocks[:, 0])
    pairs = mine.astype(jnp.float32) + to_other_core(passed).astype(jnp.float32)
    total = pick([pairs[at] for at in range(chips)], chip)
    for step in range(1, chips):
        sent = pick([pairs[at] for at in range(chips)], chip + step).astype(jnp.bfloat16)
        total = total + to_same_core(sent, step).astype(jnp.float32)
    return total


def share_of(weight_part, axis, back):
    shares = lax.axis_size("grp")
    width = weight_part.shape[axis] // shares
    index = lax.rem(lax.axis_index("grp") - back + shares, shares)
    return lax.dynamic_slice_in_dim(weight_part, index * width, width, axis).astype(jnp.bfloat16)


def ring_place(step):
    return lax.rem(lax.axis_index("fs") + step, lax.axis_size("fs"))


def exchange(share, following):
    blocks = lax.all_gather(share, "fs", axis=0, tiled=False)
    rest = jnp.stack(
        [
            lax.dynamic_index_in_dim(blocks, ring_place(step), 0, keepdims=False)
            for step in range(1, lax.axis_size("fs"))
        ]
    )
    if following is not None:
        rest, following = lax.optimization_barrier((rest, following))
    rests = [shifted(rest, "grp", back) for back in range(1, lax.axis_size("grp"))]
    return blocks, rests, following


def flat(blocks):
    return blocks.reshape((-1,) + blocks.shape[2:])


def joined(blocks, rests, locals_of):
    pieces = [flat(blocks)]
    for rest, own in zip(rests, locals_of):
        pieces += [own, flat(rest)]
    return jnp.concatenate(pieces)


def rows_in_order(normed_rows):
    shares, count = (lax.axis_size("grp"), lax.axis_size("fs"))
    rows = normed_rows.reshape(count, shares, -1, normed_rows.shape[1])

    def at(place, back):
        index = lax.rem(lax.axis_index("grp") - back + shares, shares)
        return lax.dynamic_slice(
            rows, (place, index, 0, 0), (1, 1, rows.shape[2], rows.shape[3])
        ).reshape(rows.shape[2:])

    pieces = [at(place, 0) for place in range(count)]
    for back in range(1, shares):
        pieces += [at(ring_place(step), back) for step in range(count)]
    return jnp.concatenate(pieces)


def column_terms(blocks, rests, locals_of, scale, hidden, transposed):
    shares, count = (lax.axis_size("grp"), lax.axis_size("fs"))
    place = lax.axis_index("fs")

    def product(pieces):
        form = "bnk,kt->bnt" if transposed else "bkn,kt->bnt"
        return jnp.einsum(form, pieces, hidden, preferred_element_type=jnp.float32)

    def scale_at(back):
        index = lax.rem(lax.axis_index("grp") - back + shares, shares)
        return lax.dynamic_index_in_dim(scale, index, 1, keepdims=False)[:, :, None]

    own = (product(blocks) * scale_at(0)).astype(jnp.bfloat16)
    found = [[own[at] for at in range(count)]]
    for back in range(1, shares):
        turned = scale_at(back)
        here = lax.dynamic_index_in_dim(turned, place, 0)
        local = (product(locals_of[back - 1][None]) * here).astype(jnp.bfloat16)
        away = jnp.stack(
            [
                lax.dynamic_index_in_dim(turned, ring_place(step), 0, keepdims=False)
                for step in range(1, count)
            ]
        )
        rest = (product(rests[back - 1]) * away).astype(jnp.bfloat16)
        ring = [local[0]] + [rest[at] for at in range(count - 1)]
        found.append([pick(ring, at - place) for at in range(count)])
    grp = lax.axis_index("grp")
    return [
        [pick([found[back][at] for back in range(shares)], grp - share) for share in range(shares)]
        for at in range(count)
    ]


def normed(stream, gain):
    whole_rows = gather_rows(stream)
    values = whole_rows.astype(jnp.float32)
    inverse = lax.rsqrt(jnp.mean(values * values, axis=0) + EPS)
    return (values * inverse * gain[:, None]).astype(jnp.bfloat16)


def residual(stream, total, factor):
    return (stream.astype(jnp.float32) + factor * total).astype(jnp.bfloat16)


def swish_hidden(gate, gate_scale, upward, up_scale):
    return (jax.nn.silu(gate * gate_scale[:, None]) * (upward * up_scale[:, None])).astype(
        jnp.bfloat16
    )


def gating_unit(left_pre, right_pre, channel_gain, spatial, spatial_bias):
    left = jax.nn.gelu(left_pre)
    right = jax.nn.gelu(right_pre)
    totals, squares = lax.psum((jnp.sum(right, axis=0), jnp.sum(right * right, axis=0)), "tp")
    average = totals / BRANCH
    inverse = lax.rsqrt(squares / BRANCH - average * average + EPS)
    centred = ((right - average) * inverse * channel_gain[:, None]).astype(jnp.bfloat16)
    local_groups, span = (spatial.shape[0], spatial.shape[1])
    tokens = centred.shape[1]
    blocks = centred.reshape(local_groups, centred.shape[0] // local_groups, tokens // span, span)
    target = lax.broadcasted_iota(jnp.int32, (span, span), 0)
    source = lax.broadcasted_iota(jnp.int32, (span, span), 1)
    masked = jnp.where((source <= target)[None], spatial, jnp.zeros_like(spatial))
    token_mix = jnp.einsum("gts,gcns->gcnt", masked, blocks, preferred_element_type=jnp.float32)
    token_mix = token_mix + spatial_bias[:, None, None, :]
    return (left * token_mix.reshape(centred.shape[0], tokens)).astype(jnp.bfloat16)


def layer(
    stream,
    first_gain,
    first_gate,
    first_gate_scale,
    first_up,
    first_up_scale,
    first_down,
    first_down_scale,
    mixer_gain,
    mixer_left,
    mixer_left_scale,
    mixer_right,
    mixer_right_scale,
    channel_gain,
    spatial,
    spatial_bias,
    mixer_out,
    mixer_out_scale,
    second_gain,
    second_gate,
    second_gate_scale,
    second_up,
    second_up_scale,
    second_down,
    second_down_scale,
):
    shares, count = (lax.axis_size("grp"), lax.axis_size("fs"))
    backs = range(1, shares)
    cols = lax.all_gather(
        jnp.stack([first_down_scale, mixer_out_scale, second_down_scale]), "fs", axis=0, tiled=False
    )
    cols = cols.reshape(count, 3, shares, -1)

    def mixer_share(back):
        return jnp.stack(
            [
                share_of(mixer_left, 0, back),
                share_of(mixer_right, 0, back),
                share_of(mixer_out, 1, back).T,
            ]
        )

    def rows_share(weight):
        return lambda back: share_of(weight, 0, back)

    def cols_share(weight, part, parts):
        def cut(back):
            share = share_of(weight, 1, back)
            width = share.shape[1] // parts
            return share[:, part * width : (part + 1) * width]

        return cut

    units = (
        mixer_share,
        rows_share(first_gate),
        rows_share(first_up),
        cols_share(first_down, 0, 1),
        rows_share(second_gate),
        rows_share(second_up),
    ) + tuple(cols_share(second_down, part, LAST_PARTS) for part in range(LAST_PARTS))
    ready = []
    share = units[0](0)
    for number, unit in enumerate(units):
        following = units[number + 1](0) if number + 1 < len(units) else None
        blocks, rests, share = exchange(share, following)
        ready.append((blocks, rests, [unit(back) for back in backs]))

    def half_step(stream, gain, gate_unit, gate_scale, up_unit, up_scale, down_units, down_cols):
        rows = rows_in_order(normed(stream, gain))
        gate = contract(joined(*gate_unit), rows)
        upward = contract(joined(*up_unit), rows)
        hidden = swish_hidden(gate, gate_scale, upward, up_scale)
        width = down_cols.shape[2] // len(down_units)
        terms = [
            column_terms(
                *unit, down_cols[:, :, part * width : (part + 1) * width], hidden, False
            )
            for part, unit in enumerate(down_units)
        ]
        ordered = [
            term[at][share] for at in range(count) for share in range(shares) for term in terms
        ]
        return residual(stream, scatter_blocks(jnp.concatenate(ordered)), 0.5)

    stream = half_step(
        stream, first_gain, ready[1], first_gate_scale, ready[2], first_up_scale, ready[3:4], cols[:, 0]
    )
    rows = rows_in_order(normed(stream, mixer_gain))
    blocks, rests, local_shares = ready[0]

    def mixer_unit(index):
        return (
            blocks[:, index],
            [rest[:, index] for rest in rests],
            [local_share[index] for local_share in local_shares],
        )

    left_pre = contract(joined(*mixer_unit(0)), rows)
    right_pre = contract(joined(*mixer_unit(1)), rows)
    gated = gating_unit(
        left_pre * mixer_left_scale[:, None],
        right_pre * mixer_right_scale[:, None],
        channel_gain,
        spatial,
        spatial_bias,
    )
    terms = column_terms(*mixer_unit(2), cols[:, 1], gated, True)
    terms = jnp.concatenate([terms[at][share] for at in range(count) for share in range(shares)])
    stream = residual(stream, scatter_blocks(terms), 1.0)
    return half_step(
        stream, second_gain, ready[4], second_gate_scale, ready[5], second_up_scale, ready[6:], cols[:, 2]
    )


def solution(mesh):
    return jax.shard_map(
        layer,
        mesh=mesh,
        in_specs=(
            P("tp", ("grp", "fs")),
            P(),
            P("fs", "tp"),
            P("tp"),
            P("fs", "tp"),
            P("tp"),
            P("tp", "fs"),
            P("fs"),
            P(),
            P("fs", "tp"),
            P("tp"),
            P("fs", "tp"),
            P("tp"),
            P("tp"),
            P("tp", None, None),
            P("tp", None),
            P("tp", "fs"),
            P("fs"),
            P(),
            P("fs", "tp"),
            P("tp"),
            P("fs", "tp"),
            P("tp"),
            P("tp", "fs"),
            P("fs"),
        ),
        out_specs=P("tp", ("grp", "fs")),
        check_vma=False,
    )
```
